32 devices in a mesh: grp: 2 (over x), tp: 16 (over z, y, core).
Axes of the slice: x: 2, y: 2, z: 4, core: 2. Of those that a mesh axis runs over, the one named last changes fastest.
Arguments:
- stream_in: bfloat16 [64, 4, 4096], P('grp'), parts along dimension 0, may hold values from -6 to 6
- state_in: float32 [2, 64, 8, 256, 256], P(None, 'grp', None, 'tp'), parts along dimension 1, may hold values from -0.8 to 0.8
- norm_gain: bfloat16 [2, 4096], replicated, may hold values from 0.099609375 to 1.8984375
- query_weight: bfloat16 [2, 4096, 2048], P(None, None, 'tp'), may hold values from -0.09375 to 0.09375
- key_weight: bfloat16 [2, 4096, 2048], P(None, None, 'tp'), may hold values from -0.09375 to 0.09375
- value_weight: bfloat16 [2, 4096, 8, 256], P(None, None, None, 'tp'), as said below
- gate_weight: bfloat16 [2, 4096, 8, 256], P(None, None, None, 'tp'), may hold values from -0.09375 to 0.09375
- group_gain: bfloat16 [2, 8, 256], P(None, None, 'tp'), may hold values from 0.099609375 to 1.8984375
- output_weight: bfloat16 [2, 8, 256, 4096], P(None, None, 'tp'), may hold values from -0.375 to 0.375
Outputs:
- stream_out: bfloat16 [64, 4, 4096], P('grp', None, 'tp'), parts along dimension 0
- state_out: float32 [2, 64, 8, 256, 256], P(None, 'grp', None, 'tp'), parts along dimension 1
The draws below stay inside these ranges and needn't reach their ends.
There are 2 independent parts, one for each index of `grp`. The reference program is written for one: setup_inputs(seed, part) draws one part's arguments, and reference() takes and returns one part's arrays. A program takes and returns all parts, laid end to end along the dimension named above; an argument that names none is the same for every part. Nothing has to cross between parts.
Inputs may be any that keep to these rules, and one draw needn't show every extreme that they name: `value_weight`: real values; column scales of the value projection differ.
All inputs are finite; a program needn't handle non-finite values.
Results may differ from the reference program's by a relative error of at most 0.024.
Values may be sent and summed in bfloat16 or wider, within the bound.
A program may use at most 64 MiB of HBM per device.

```python
import jax
import jax.numpy as jnp
from jax import lax

D = 4096
HEADS = 8
HEAD_DIM = 256
SEQS = 32
NEW_TOK = 4
PAST = 1024
LAYERS = 2


def draw_value_weight(key, part):
    first_key, second_key = jax.random.split(jax.random.fold_in(key, 17))
    base = jax.random.normal(first_key, (LAYERS, D, HEADS, HEAD_DIM), jnp.float32) * D ** (-0.5)
    ramp = jnp.arange(HEAD_DIM, dtype=jnp.float32) / (HEAD_DIM - 1)
    rough = jax.random.uniform(second_key, (LAYERS, 1, HEADS, HEAD_DIM), jnp.float32, -0.4, 0.4)
    scales = jnp.power(3.0, ramp) * jnp.exp(rough)
    return (base * scales).astype(jnp.bfloat16)


def strengthened(drawn, key, source, target, shards_of, factor):
    def block_of(dim):
        return (jnp.arange(drawn.shape[dim]) // (drawn.shape[dim] // shards_of)).reshape((-1,) + (1,) * (drawn.ndim - 1 - dim))

    near = jax.random.permutation(key, shards_of)[block_of(target)]
    far = (block_of(target) + shards_of // 2) % shards_of
    return jnp.where((block_of(source) == near) | (block_of(source) == far), factor * drawn, drawn)


def level_of(own_key, dims, cuts, smallest, largest):
    loudness, own = 1.0, jax.random.fold_in(own_key, 6)
    for position, blocks in cuts:
        steps = jnp.exp(jax.random.uniform(jax.random.fold_in(own, position), (blocks,), jnp.float32, smallest / len(cuts), largest / len(cuts)))
        loudness = loudness * jnp.repeat(steps, dims[position] // blocks).reshape([-1 if axis == position else 1 for axis in range(len(dims))])
    return loudness


def bell_draw(own_key, shape, scale, most, pieces=(), held_as=jnp.bfloat16):
    factor_of = level_of(own_key, shape, pieces, -0.22, 0.18) if pieces else 1.0
    drawn = jax.random.normal(own_key, shape, jnp.float32) * scale * factor_of
    return jnp.minimum(jnp.maximum(drawn, -most), most).astype(held_as)


def heavy_noise(rng, dims, spread, most, shards, heavy, kind=jnp.bfloat16):
    array = spread * jax.random.normal(rng, dims, jnp.float32)
    if shards:
        array = array * level_of(rng, dims, shards, -0.22, 0.18)
    return jnp.clip(strengthened(array, jax.random.fold_in(rng, 3), *heavy), -most, most).astype(kind)


def setup_inputs(seed: int = 0, part: int = 0) -> dict:
    key_of = jax.random.split(jax.random.key(seed), 10)
    part_splits = jax.random.split(jax.random.fold_in(key_of[9], part), 10)
    return {
        "stream_in": bell_draw(part_splits[0], (SEQS, NEW_TOK, D), 1.0, 6.0),
        "state_in": bell_draw(part_splits[1], (LAYERS, SEQS, HEADS, HEAD_DIM, HEAD_DIM), 0.1, 0.8, ((3, 16),), jnp.float32),
        "norm_gain": jnp.clip(1.0 + 0.18 * jax.random.normal(key_of[2], (LAYERS, D), jnp.float32), 0.099609375, 1.8984375).astype(jnp.bfloat16),
        "query_weight": bell_draw(key_of[3], (LAYERS, D, HEADS * HEAD_DIM), D ** -0.5, 0.09375, ((2, 16),)),
        "key_weight": bell_draw(key_of[4], (LAYERS, D, HEADS * HEAD_DIM), D ** -0.5, 0.09375, ((2, 16),)),
        "value_weight": draw_value_weight(jax.random.fold_in(key_of[9], 71), part),
        "gate_weight": bell_draw(key_of[6], (LAYERS, D, HEADS, HEAD_DIM), D ** -0.5, 0.09375, ((3, 16),)),
        "group_gain": jnp.clip(1.0 + 0.18 * jax.random.normal(key_of[7], (LAYERS, HEADS, HEAD_DIM), jnp.float32), 0.099609375, 1.8984375).astype(jnp.bfloat16),
        "output_weight": heavy_noise(key_of[8], (LAYERS, HEADS, HEAD_DIM, D), (HEADS * HEAD_DIM // 4) ** -0.5, 0.375, ((2, 16),), (2, 3, 16, 2.0)),
    }


EPS_RMS = 1e-06
EPS_GROUP = 1e-05
ROTARY_BASE = 10000.0

def log_decays(count):
    return jnp.log(1.0 - jnp.power(2.0, -5.0 - jnp.arange(count, dtype=jnp.float32)))

def decay_tables(log_gamma, count):
    steps = jnp.arange(count, dtype=jnp.float32)
    gap = steps[:, None] - steps[None, :]
    intra = jnp.where(gap[None] >= 0, jnp.exp(log_gamma[:, None, None] * jnp.maximum(gap, 0.0)[None]), 0.0)
    q_decay = jnp.exp(log_gamma[None, :] * (steps[:, None] + 1.0))
    k_decay = jnp.exp(log_gamma[None, :] * (count - 1.0 - steps[:, None]))
    block_decay = jnp.exp(log_gamma * count)
    return (intra, q_decay, k_decay, block_decay)

def rotate(values, offset):
    half_dim = values.shape[-1] // 2
    freqs = jnp.power(ROTARY_BASE, -jnp.arange(half_dim, dtype=jnp.float32) * (2.0 / values.shape[-1]))
    places = (offset + jnp.arange(values.shape[1])).astype(jnp.float32)
    angles = places[:, None] * freqs[None, :]
    cosine = jnp.cos(angles)[None, :, None, :]
    sine = jnp.sin(angles)[None, :, None, :]
    first = values[..., :half_dim]
    second = values[..., half_dim:]
    return jnp.concatenate([first * cosine - second * sine, second * cosine + first * sine], axis=-1)

def reference(stream_in, state_in, norm_gain, query_weight, key_weight, value_weight, gate_weight, group_gain, output_weight):
    seqs, new_tok, width = stream_in.shape
    heads, head_dim = (value_weight.shape[2], value_weight.shape[3])
    log_gamma = log_decays(heads)
    intra, q_decay, k_decay, block_decay = decay_tables(log_gamma, new_tok)
    highest = lax.Precision.HIGHEST
    stream = stream_in
    new_states = []
    for layer_no in range(state_in.shape[0]):
        stream_f = stream.astype(jnp.float32)
        normed = stream_f * lax.rsqrt(lax.optimization_barrier(jnp.mean(stream_f * stream_f, axis=-1, keepdims=True)) + EPS_RMS)
        normed = (normed * norm_gain[layer_no].astype(jnp.float32)).astype(jnp.bfloat16)
        flat = normed.reshape(seqs * new_tok, width)

        def project(weight):
            result = jnp.dot(flat, weight.reshape(width, heads * head_dim), preferred_element_type=jnp.float32)
            result = lax.optimization_barrier(result.astype(jnp.bfloat16))
            return result.astype(jnp.float32).reshape(seqs, new_tok, heads, head_dim)
        queries = project(query_weight[layer_no])
        key_rows = project(key_weight[layer_no])
        values_f = project(value_weight[layer_no])
        gates_f = project(gate_weight[layer_no])
        rot_q = rotate(queries, PAST)
        rot_k = rotate(key_rows, PAST) * head_dim ** (-0.5)
        scores = jnp.einsum('bthd,bshd->bhts', rot_q, rot_k, precision=highest) * intra[None]
        inner = jnp.einsum('bhts,bshe->bthe', scores, values_f, precision=highest)
        state = state_in[layer_no]
        carried = jnp.einsum('bthd,bhed->bthe', rot_q, state, precision=highest) * q_decay[None, :, :, None]
        mixed = inner + carried
        new_state = state * block_decay[None, :, None, None] + jnp.einsum('bthe,bthd->bhed', values_f, rot_k * k_decay[None, :, :, None], precision=highest)
        mean_o = lax.optimization_barrier(jnp.mean(mixed, axis=-1, keepdims=True))
        var_o = lax.optimization_barrier(jnp.mean(jnp.square(mixed - mean_o), axis=-1, keepdims=True))
        normal = (mixed - mean_o) * lax.rsqrt(var_o + EPS_GROUP) * group_gain[layer_no].astype(jnp.float32)[None, None]
        gated = (jax.nn.silu(gates_f) * normal).astype(jnp.bfloat16)
        branch = jnp.dot(gated.reshape(seqs * new_tok, heads * head_dim), output_weight[layer_no].reshape(heads * head_dim, width), preferred_element_type=jnp.float32)
        stream = (stream.astype(jnp.float32) + branch.reshape(seqs, new_tok, width)).astype(jnp.bfloat16)
        new_states.append(new_state)
    return (stream, jnp.stack(new_states))
```

```python
import functools

import jax
import jax.numpy as jnp
import numpy as np
from jax import lax
from jax.experimental import pallas as pl
from jax.experimental.pallas import tpu as pltpu
from jax.sharding import PartitionSpec as P

HEAD_DIM = 256
PAST = 1024


EPS_RMS = 1e-06
EPS_GROUP = 1e-05
ROTARY_BASE = 10000.0


def log_decays(count):
    return jnp.log(1.0 - jnp.power(2.0, -5.0 - jnp.arange(count, dtype=jnp.float32)))


def decay_tables(log_gamma, count):
    steps = jnp.arange(count, dtype=jnp.float32)
    gap = steps[:, None] - steps[None, :]
    intra = jnp.where(
        gap[None] >= 0, jnp.exp(log_gamma[:, None, None] * jnp.maximum(gap, 0.0)[None]), 0.0
    )
    q_decay = jnp.exp(log_gamma[None, :] * (steps[:, None] + 1.0))
    k_decay = jnp.exp(log_gamma[None, :] * (count - 1.0 - steps[:, None]))
    block_decay = jnp.exp(log_gamma * count)
    return (intra, q_decay, k_decay, block_decay)


def rotate(values, offset):
    half_dim = values.shape[-1] // 2
    freqs = jnp.power(
        ROTARY_BASE, -jnp.arange(half_dim, dtype=jnp.float32) * (2.0 / values.shape[-1])
    )
    places = (offset + jnp.arange(values.shape[1])).astype(jnp.float32)
    angles = places[:, None] * freqs[None, :]
    cosine = jnp.cos(angles)[None, :, None, :]
    sine = jnp.sin(angles)[None, :, None, :]
    first = values[..., :half_dim]
    second = values[..., half_dim:]
    return jnp.concatenate(
        [first * cosine - second * sine, second * cosine + first * sine], axis=-1
    )


def plain_local(
    stream_in,
    state_in,
    norm_gain,
    query_weight,
    key_weight,
    value_weight,
    gate_weight,
    group_gain,
    output_weight,
):
    seqs, new_tok, width = stream_in.shape
    heads, local_dim = (value_weight.shape[2], value_weight.shape[3])
    head_dim = HEAD_DIM
    log_gamma = log_decays(heads)
    intra, q_decay, k_decay, block_decay = decay_tables(log_gamma, new_tok)
    highest = lax.Precision.HIGHEST
    share_cols = width // lax.axis_size("tp")
    col_start = lax.axis_index("tp") * share_cols
    layers = state_in.shape[0]
    stream = stream_in
    stream_share = stream_in
    new_states = []
    for layer_no in range(layers):
        stream_f = stream.astype(jnp.float32)
        normed = stream_f * lax.rsqrt(
            jnp.mean(stream_f * stream_f, axis=-1, keepdims=True) + EPS_RMS
        )
        normed = (normed * norm_gain[layer_no].astype(jnp.float32)).astype(jnp.bfloat16)
        flat = normed.reshape(seqs * new_tok, width)
        query_part = jnp.dot(flat, query_weight[layer_no], preferred_element_type=jnp.float32)
        query_part = query_part.astype(jnp.bfloat16).reshape(seqs, new_tok, -1)
        key_part = jnp.dot(flat, key_weight[layer_no], preferred_element_type=jnp.float32)
        key_part = key_part.astype(jnp.bfloat16).reshape(seqs, new_tok, -1)

        def project_local(weight):
            result = jnp.dot(
                flat, weight.reshape(width, heads * local_dim), preferred_element_type=jnp.float32
            )
            result = lax.optimization_barrier(result.astype(jnp.bfloat16))
            return result.astype(jnp.float32).reshape(seqs, new_tok, heads, local_dim)

        values_f = project_local(value_weight[layer_no])
        gates_f = project_local(gate_weight[layer_no])
        queries, key_rows = (
            lax.all_gather(query_part, "tp", axis=2, tiled=True),
            lax.all_gather(key_part, "tp", axis=2, tiled=True),
        )
        queries = queries.astype(jnp.float32).reshape(seqs, new_tok, heads, head_dim)
        key_rows = key_rows.astype(jnp.float32).reshape(seqs, new_tok, heads, head_dim)
        rot_q = rotate(queries, PAST)
        rot_k = rotate(key_rows, PAST) * head_dim ** (-0.5)
        scores = jnp.einsum("bthd,bshd->bhts", rot_q, rot_k, precision=highest) * intra[None]
        inner = jnp.einsum("bhts,bshe->bthe", scores, values_f, precision=highest)
        state = state_in[layer_no]
        carried = (
            jnp.einsum("bthd,bhed->bthe", rot_q, state, precision=highest)
            * q_decay[None, :, :, None]
        )
        mixed = inner + carried
        new_state = state * block_decay[None, :, None, None] + jnp.einsum(
            "bthe,bthd->bhed", values_f, rot_k * k_decay[None, :, :, None], precision=highest
        )
        new_states.append(new_state)
        totals, squares = lax.psum((jnp.sum(mixed, axis=-1), jnp.sum(mixed * mixed, axis=-1)), "tp")
        mean_o = (totals / head_dim)[..., None]
        var_o = (squares / head_dim)[..., None] - mean_o * mean_o
        normal = (
            (mixed - mean_o)
            * lax.rsqrt(var_o + EPS_GROUP)
            * group_gain[layer_no].astype(jnp.float32)[None, None]
        )
        gated = (jax.nn.silu(gates_f) * normal).astype(jnp.bfloat16)
        partial_out = jnp.dot(
            gated.reshape(seqs * new_tok, heads * local_dim),
            output_weight[layer_no].reshape(heads * local_dim, width),
            preferred_element_type=jnp.float32,
        ).reshape(seqs, new_tok, width)
        share_out = lax.psum_scatter(partial_out, "tp", scatter_dimension=2, tiled=True)
        own_cols = lax.dynamic_slice_in_dim(stream, col_start, share_cols, 2)
        stream_share = (own_cols.astype(jnp.float32) + share_out).astype(jnp.bfloat16)
        if layer_no + 1 < layers:
            stream = lax.all_gather(stream_share, "tp", axis=2, tiled=True)
    result = stream_share
    return (result, jnp.stack(new_states))


F32 = jnp.float32
BF16 = jnp.bfloat16


def nt_dot(a, b, precision=None):
    return lax.dot_general(
        a, b, (((1,), (1,)), ((), ())), preferred_element_type=F32, precision=precision
    )


def log2(value):
    return int(value).bit_length() - 1


def rotary_tables(heads, new_tok, head_dim):
    half = head_dim // 2
    freqs = np.power(
        np.float32(ROTARY_BASE), -np.arange(half, dtype=np.float32) * np.float32(2.0 / head_dim)
    ).astype(np.float32)
    tok = np.arange(8) % new_tok
    places = (PAST + tok).astype(np.float32)
    angles = (places[:, None] * freqs[None, :]).astype(np.float32).astype(np.float64)
    gamma = 1.0 - np.power(2.0, -5.0 - np.arange(heads))
    grow = np.power(gamma[:, None], tok[None, :] + 1.0)[:, :, None]
    shrink = head_dim ** (-0.5) / grow
    cosine, sine = np.cos(angles)[None], np.sin(angles)[None]
    block = np.broadcast_to(np.power(gamma, new_tok)[:, None, None], (heads, 8, half))
    return np.stack(
        [cosine * grow, sine * grow, cosine * shrink, sine * shrink, block]
    ).astype(np.float32)


def kernel(
    n, head_dim,
    x_hbm, st_hbm, ng_ref, qw_hbm, kw_hbm, vw_hbm, gw_hbm, gg_ref, ow_hbm, tab_ref,
    y_ref, so_hbm,
    xs, nv, wqk, wvg, wo, stv, qkg, kh, vts, sb, pbs, pbr, rss, rsr, mkc, mks, fold,
    lsem, ag_s, ag_r, st_s, st_r, pb_s, pb_r, rs_s, rs_r, osem,
):
    layers, seqs, heads, e_dim, _ = st_hbm.shape
    rows, width = x_hbm.shape
    tok = rows // seqs
    share = width // n
    cols = qw_hbm.shape[2]
    he = heads * e_dim
    half = head_dim // 2
    nc = n // 2
    me = lax.axis_index("tp")
    core = lax.rem(me, 2)
    chip = lax.div(me, 2)
    partner = chip * 2 + 1 - core

    def away(o, c):
        return lax.rem(chip + o, nc) * 2 + c

    def back(o, c):
        return lax.rem(chip - o + nc, nc) * 2 + c

    def remote(src, dst, ssem, rsem, device):
        return pltpu.make_async_remote_copy(
            src_ref=src, dst_ref=dst, send_sem=ssem, recv_sem=rsem,
            device_id={"tp": device}, device_id_type=pl.DeviceIdType.MESH,
        )

    loads = {}
    count = 0

    def load(name, src, dst):
        nonlocal count
        loads[name] = pltpu.make_async_copy(src, dst, lsem.at[count])
        loads[name].start()
        count += 1

    for j in range(n):
        load(("x", j), x_hbm.at[:, pl.ds(j * share, share)], xs.at[0, j])
    for l in range(layers):
        load(("q", l), qw_hbm.at[l], wqk.at[l, :, pl.ds(0, cols)])
        load(("k", l), kw_hbm.at[l], wqk.at[l, :, pl.ds(cols, cols)])
        load(("v", l), vw_hbm.at[l], wvg.at[l, pl.ds(0, he)])
        load(("g", l), gw_hbm.at[l], wvg.at[l, pl.ds(he, he)])
        load(("s", l), st_hbm.at[l], stv.at[l])
        load(("o", l), ow_hbm.at[l], wo.at[l])

    barrier = pltpu.get_barrier_semaphore()
    for o in range(1, n):
        pl.semaphore_signal(
            barrier, inc=1, device_id={"tp": lax.rem(me + o, n)},
            device_id_type=pl.DeviceIdType.MESH,
        )

    be = seqs * e_dim

    def iota(shape, dim, shift=0):
        return jnp.right_shift(lax.broadcasted_iota(jnp.int32, shape, dim), shift)

    te, tt = log2(e_dim), log2(tok)
    mkc[...] = (iota((rows, be), 0, tt) == iota((rows, be), 1, te)).astype(F32).astype(BF16)
    mks[...] = (iota((be, rows), 0, te) == iota((be, rows), 1, tt)).astype(F32).astype(BF16)
    low = e_dim - 1
    fold[...] = (
        jnp.bitwise_and(iota((be, he), 0), low) == jnp.bitwise_and(iota((be, he), 1), low)
    ).astype(F32).astype(BF16)
    causal = (
        (iota((rows, rows), 0, tt) == iota((rows, rows), 1, tt))
        & (iota((rows, rows), 0) >= iota((rows, rows), 1))
    ).astype(F32)
    heads_of = (iota((heads, he), 0) == iota((heads, he), 1, te)).astype(F32)
    place = (
        iota((e_dim, he), 0) == jnp.bitwise_and(iota((e_dim, he), 1), low)
    ).astype(F32)
    highest = lax.Precision.HIGHEST

    def gather_start(buf, p):
        sent = []
        for o in range(1, nc):
            sent.append(remote(buf.at[me], buf.at[me], ag_s.at[p, o], ag_r.at[p, o], away(o, core)))
        sent.append(remote(buf.at[me], buf.at[me], ag_s.at[p, nc], ag_r.at[p, nc], partner))
        for copy in sent:
            copy.start()
        return sent

    def gather_finish(buf, p, sent):
        for o in range(1, nc):
            slot = buf.at[back(o, core)]
            remote(slot, slot, ag_s.at[p, o], ag_r.at[p, o], partner).wait_recv()
            copy = remote(slot, slot, ag_s.at[p, nc + o], ag_r.at[p, nc + o], partner)
            copy.start()
            sent.append(copy)
        for o in range(nc):
            slot = buf.at[back(o, 1 - core)]
            remote(slot, slot, ag_s.at[p, nc + o], ag_r.at[p, nc + o], partner).wait_recv()

    def spread(table):
        return jnp.broadcast_to(table[None], (rows // 8, 8, half)).reshape(rows, half)

    started = []
    outs = []
    for l in range(layers):
        if l == 0:
            for j in range(n):
                loads[("x", j)].wait()

        def square(j, acc):
            block = xs[l, j].astype(F32)
            return acc + block * block

        total = lax.fori_loop(0, n, square, jnp.zeros((rows, share), F32))
        scale = lax.rsqrt(jnp.sum(total, axis=1, keepdims=True) / width + EPS_RMS)

        def normalise(j, carry):
            at = pl.ds(pl.multiple_of(j * share, share), share)
            gain = ng_ref[l : l + 1, at].astype(F32)
            nv[:, at] = (xs[l, j].astype(F32) * scale * gain).astype(BF16)
            return carry

        lax.fori_loop(0, n, normalise, 0)
        loads[("q", l)].wait()
        loads[("k", l)].wait()
        qkg[l, me] = jnp.dot(nv[...], wqk[l], preferred_element_type=F32).astype(BF16)
        if l == 0:
            pl.semaphore_wait(barrier, n - 1)
        sent = gather_start(qkg.at[l], 2 * l)
        loads[("v", l)].wait()
        loads[("g", l)].wait()
        vg = nt_dot(nv[...], wvg[l])
        values = vg[:, :he].astype(BF16)
        gates = vg[:, he:].astype(BF16).astype(F32)
        vts[...] = jnp.transpose(values.astype(F32)).astype(BF16)
        loads[("s", l)].wait()
        gather_finish(qkg.at[l], 2 * l, sent)
        started += sent

        def mix(h, acc):
            qk_a = qkg[l, 2 * h].astype(F32)
            qk_b = qkg[l, 2 * h + 1].astype(F32)
            qa, ka = qk_a[:, :half], qk_a[:, half:]
            qb, kb = qk_b[:, :half], qk_b[:, half:]
            cq, sq = spread(tab_ref[0, h]), spread(tab_ref[1, h])
            ck, sk = spread(tab_ref[2, h]), spread(tab_ref[3, h])
            rq = jnp.concatenate([qa * cq - qb * sq, qb * cq + qa * sq], axis=1).astype(BF16)
            rk = jnp.concatenate([ka * ck - kb * sk, kb * ck + ka * sk], axis=1).astype(BF16)
            kh[h] = rk
            state = stv[l, :, h].reshape(be, head_dim).astype(BF16)
            scores = (nt_dot(rq, rk) * causal).astype(BF16)
            carried = nt_dot(rq, state).astype(BF16) * mkc[...]
            part = jnp.dot(scores, values, preferred_element_type=F32)
            part = part + jnp.dot(carried, fold[...], preferred_element_type=F32)
            own = (iota((1, he), 1, te) == h).astype(F32)
            return acc + part * own

        mixed = lax.fori_loop(0, heads, mix, jnp.zeros((rows, he), F32))
        sums = nt_dot(heads_of, mixed, highest)
        squares = nt_dot(heads_of, mixed * mixed, highest)
        sb[l, me] = jnp.concatenate([sums, squares], axis=0)
        sent = []
        for o in range(1, n):
            sent.append(
                remote(sb.at[l, me], sb.at[l, me], st_s.at[l, o], st_r.at[l, o], lax.rem(me + o, n))
            )
        for copy in sent:
            copy.start()
        started += sent

        def update(h, carry):
            at = pl.ds(pl.multiple_of(h * e_dim, e_dim), e_dim)
            tall = jnp.broadcast_to(vts[at, :][None], (seqs, e_dim, rows)).reshape(be, rows)
            fresh = jnp.dot(tall * mks[...], kh[h], preferred_element_type=F32)
            row = tab_ref[4, h][0:1, :]
            fade = jnp.concatenate([row, row], axis=1)
            state = stv[l, :, h].reshape(be, head_dim)
            stv[l, :, h] = ((state + fresh) * fade).reshape(seqs, e_dim, head_dim)
            return carry

        lax.fori_loop(0, heads, update, 0)

        for o in range(1, n):
            slot = sb.at[l, lax.rem(me - o + n, n)]
            remote(slot, slot, st_s.at[l, o], st_r.at[l, o], partner).wait_recv()
        out = pltpu.make_async_copy(stv.at[l], so_hbm.at[l], osem.at[l])
        out.start()
        outs.append(out)
        stats = jnp.sum(sb[l], axis=0)
        mean = stats[:heads] / head_dim
        var = stats[heads:] / head_dim - mean * mean
        rstd = lax.rsqrt(var + EPS_GROUP)

        def expand(small):
            return lax.dot_general(
                small, heads_of, (((0,), (0,)), ((), ())),
                preferred_element_type=F32, precision=highest,
            )

        gain = jnp.dot(gg_ref[l].astype(F32), place, preferred_element_type=F32, precision=highest)
        gain = jnp.sum(gain * heads_of, axis=0, keepdims=True)
        normal = (mixed - expand(mean)) * expand(rstd) * gain
        gated = (gates / (1.0 + jnp.exp(-gates)) * normal).astype(BF16)

        loads[("o", l)].wait()

        def chunk(j):
            at = pl.ds(pl.multiple_of(j * share, share), share)
            return jnp.dot(gated, wo[l, :, at], preferred_element_type=F32)

        order = list(range(1, nc)) + [0]
        for o in order:
            pbs[l, o] = chunk(away(o, 1 - core)).astype(BF16)
            copy = remote(pbs.at[l, o], pbr.at[l, o], pb_s.at[l, o], pb_r.at[l, o], partner)
            copy.start()
            started.append(copy)
        acc = None
        for o in order:
            own = chunk(away(o, core))
            remote(pbs.at[l, o], pbr.at[l, o], pb_s.at[l, o], pb_r.at[l, o], partner).wait_recv()
            own = own + pbr[l, o].astype(F32)
            if o:
                rss[l, o] = own.astype(BF16)
                copy = remote(rss.at[l, o], rsr.at[l, o], rs_s.at[l, o], rs_r.at[l, o], away(o, core))
                copy.start()
                started.append(copy)
            else:
                acc = own
        for o in range(1, nc):
            remote(rss.at[l, o], rsr.at[l, o], rs_s.at[l, o], rs_r.at[l, o], partner).wait_recv()
            acc = acc + rsr[l, o].astype(F32)
        fresh_x = (xs[l, me].astype(F32) + acc).astype(BF16)
        if l + 1 < layers:
            xs[l + 1, me] = fresh_x
            sent = gather_start(xs.at[l + 1], 2 * l + 1)
            gather_finish(xs.at[l + 1], 2 * l + 1, sent)
            started += sent
        else:
            y_ref[...] = fresh_x
    for copy in started:
        copy.wait_send()
    for copy in outs:
        copy.wait()


def local(
    stream_in, state_in, norm_gain, query_weight, key_weight,
    value_weight, gate_weight, group_gain, output_weight,
):
    n = lax.axis_size("tp")
    seqs, tok, width = stream_in.shape
    layers, _, heads, e_dim, head_dim = state_in.shape
    cols = query_weight.shape[2]
    rows = seqs * tok
    he = heads * e_dim
    share = width // n
    fits = (
        cols == 128 and head_dim == 256 and he == 128 and heads == 8 and e_dim == 16
        and share % 128 == 0 and n % 2 == 0 and rows == 128 and 8 % tok == 0
    )
    if not fits:
        return plain_local(
            stream_in, state_in, norm_gain, query_weight, key_weight,
            value_weight, gate_weight, group_gain, output_weight,
        )
    nc = n // 2
    be = seqs * e_dim
    hbm = pl.BlockSpec(memory_space=pl.ANY)
    vmem = pl.BlockSpec(memory_space=pltpu.VMEM)
    dma = pltpu.SemaphoreType.DMA
    tables = jnp.asarray(rotary_tables(heads, tok, head_dim))
    flat = lambda w: jnp.transpose(w, (0, 2, 3, 1)).reshape(layers, he, width)
    y, new_state = pl.pallas_call(
        functools.partial(kernel, n, head_dim),
        name="retention",
        out_shape=(
            jax.ShapeDtypeStruct((rows, share), BF16),
            jax.ShapeDtypeStruct(state_in.shape, F32),
        ),
        in_specs=[hbm, hbm, vmem, hbm, hbm, hbm, hbm, vmem, hbm, vmem],
        out_specs=(vmem, hbm),
        scratch_shapes=[
            pltpu.VMEM((layers, n, rows, share), BF16),
            pltpu.VMEM((rows, width), BF16),
            pltpu.VMEM((layers, width, 2 * cols), BF16),
            pltpu.VMEM((layers, 2 * he, width), BF16),
            pltpu.VMEM((layers, he, width), BF16),
            pltpu.VMEM(state_in.shape, F32),
            pltpu.VMEM((layers, n, rows, 2 * cols), BF16),
            pltpu.VMEM((heads, rows, head_dim), BF16),
            pltpu.VMEM((he, rows), BF16),
            pltpu.VMEM((layers, n, 2 * heads, rows), F32),
            pltpu.VMEM((layers, nc, rows, share), BF16),
            pltpu.VMEM((layers, nc, rows, share), BF16),
            pltpu.VMEM((layers, nc, rows, share), BF16),
            pltpu.VMEM((layers, nc, rows, share), BF16),
            pltpu.VMEM((rows, be), BF16),
            pltpu.VMEM((be, rows), BF16),
            pltpu.VMEM((be, he), BF16),
            dma((n + 6 * layers,)),
            dma((2 * layers, n)),
            dma((2 * layers, n)),
            dma((layers, n)),
            dma((layers, n)),
            dma((layers, nc)),
            dma((layers, nc)),
            dma((layers, nc)),
            dma((layers, nc)),
            dma((layers,)),
        ],
        compiler_params=pltpu.CompilerParams(
            collective_id=0, has_side_effects=True, vmem_limit_bytes=60 * 2**20
        ),
    )(
        stream_in.reshape(rows, width), state_in, norm_gain, query_weight, key_weight,
        flat(value_weight), flat(gate_weight), group_gain,
        output_weight.reshape(layers, he, width), tables,
    )
    return y.reshape(seqs, tok, share), new_state


def solution(mesh):
    in_specs = (
        P("grp", None, None),
        P(None, "grp", None, "tp", None),
        P(),
        P(None, None, "tp"),
        P(None, None, "tp"),
        P(None, None, None, "tp"),
        P(None, None, None, "tp"),
        P(None, None, "tp"),
        P(None, None, "tp", None),
    )
    out_specs = (P("grp", None, "tp"), P(None, "grp", None, "tp", None))
    return jax.shard_map(local, mesh=mesh, in_specs=in_specs, out_specs=out_specs, check_vma=False)
```

```python
import functools

import jax
import jax.numpy as jnp
import numpy as np
from jax import lax
from jax.experimental import pallas as pl
from jax.experimental.pallas import tpu as pltpu
from jax.sharding import PartitionSpec as P

HEAD_DIM = 256
PAST = 1024


EPS_RMS = 1e-06
EPS_GROUP = 1e-05
ROTARY_BASE = 10000.0


def log_decays(count):
    return jnp.log(1.0 - jnp.power(2.0, -5.0 - jnp.arange(count, dtype=jnp.float32)))


def decay_tables(log_gamma, count):
    steps = jnp.arange(count, dtype=jnp.float32)
    gap = steps[:, None] - steps[None, :]
    intra = jnp.where(
        gap[None] >= 0, jnp.exp(log_gamma[:, None, None] * jnp.maximum(gap, 0.0)[None]), 0.0
    )
    q_decay = jnp.exp(log_gamma[None, :] * (steps[:, None] + 1.0))
    k_decay = jnp.exp(log_gamma[None, :] * (count - 1.0 - steps[:, None]))
    block_decay = jnp.exp(log_gamma * count)
    return (intra, q_decay, k_decay, block_decay)


def rotate(values, offset):
    half_dim = values.shape[-1] // 2
    freqs = jnp.power(
        ROTARY_BASE, -jnp.arange(half_dim, dtype=jnp.float32) * (2.0 / values.shape[-1])
    )
    places = (offset + jnp.arange(values.shape[1])).astype(jnp.float32)
    angles = places[:, None] * freqs[None, :]
    cosine = jnp.cos(angles)[None, :, None, :]
    sine = jnp.sin(angles)[None, :, None, :]
    first = values[..., :half_dim]
    second = values[..., half_dim:]
    return jnp.concatenate(
        [first * cosine - second * sine, second * cosine + first * sine], axis=-1
    )


def plain_local(
    stream_in,
    state_in,
    norm_gain,
    query_weight,
    key_weight,
    value_weight,
    gate_weight,
    group_gain,
    output_weight,
):
    seqs, new_tok, width = stream_in.shape
    heads, local_dim = (value_weight.shape[2], value_weight.shape[3])
    head_dim = HEAD_DIM
    log_gamma = log_decays(heads)
    intra, q_decay, k_decay, block_decay = decay_tables(log_gamma, new_tok)
    highest = lax.Precision.HIGHEST
    share_cols = width // lax.axis_size("tp")
    col_start = lax.axis_index("tp") * share_cols
    layers = state_in.shape[0]
    stream = stream_in
    stream_share = stream_in
    new_states = []
    for layer_no in range(layers):
        stream_f = stream.astype(jnp.float32)
        normed = stream_f * lax.rsqrt(
            jnp.mean(stream_f * stream_f, axis=-1, keepdims=True) + EPS_RMS
        )
        normed = (normed * norm_gain[layer_no].astype(jnp.float32)).astype(jnp.bfloat16)
        flat = normed.reshape(seqs * new_tok, width)
        query_part = jnp.dot(flat, query_weight[layer_no], preferred_element_type=jnp.float32)
        query_part = query_part.astype(jnp.bfloat16).reshape(seqs, new_tok, -1)
        key_part = jnp.dot(flat, key_weight[layer_no], preferred_element_type=jnp.float32)
        key_part = key_part.astype(jnp.bfloat16).reshape(seqs, new_tok, -1)

        def project_local(weight):
            result = jnp.dot(
                flat, weight.reshape(width, heads * local_dim), preferred_element_type=jnp.float32
            )
            result = lax.optimization_barrier(result.astype(jnp.bfloat16))
            return result.astype(jnp.float32).reshape(seqs, new_tok, heads, local_dim)

        values_f = project_local(value_weight[layer_no])
        gates_f = project_local(gate_weight[layer_no])
        queries, key_rows = (
            lax.all_gather(query_part, "tp", axis=2, tiled=True),
            lax.all_gather(key_part, "tp", axis=2, tiled=True),
        )
        queries = queries.astype(jnp.float32).reshape(seqs, new_tok, heads, head_dim)
        key_rows = key_rows.astype(jnp.float32).reshape(seqs, new_tok, heads, head_dim)
        rot_q = rotate(queries, PAST)
        rot_k = rotate(key_rows, PAST) * head_dim ** (-0.5)
        scores = jnp.einsum("bthd,bshd->bhts", rot_q, rot_k, precision=highest) * intra[None]
        inner = jnp.einsum("bhts,bshe->bthe", scores, values_f, precision=highest)
        state = state_in[layer_no]
        carried = (
            jnp.einsum("bthd,bhed->bthe", rot_q, state, precision=highest)
            * q_decay[None, :, :, None]
        )
        mixed = inner + carried
        new_state = state * block_decay[None, :, None, None] + jnp.einsum(
            "bthe,bthd->bhed", values_f, rot_k * k_decay[None, :, :, None], precision=highest
        )
        new_states.append(new_state)
        totals, squares = lax.psum((jnp.sum(mixed, axis=-1), jnp.sum(mixed * mixed, axis=-1)), "tp")
        mean_o = (totals / head_dim)[..., None]
        var_o = (squares / head_dim)[..., None] - mean_o * mean_o
        normal = (
            (mixed - mean_o)
            * lax.rsqrt(var_o + EPS_GROUP)
            * group_gain[layer_no].astype(jnp.float32)[None, None]
        )
        gated = (jax.nn.silu(gates_f) * normal).astype(jnp.bfloat16)
        partial_out = jnp.dot(
            gated.reshape(seqs * new_tok, heads * local_dim),
            output_weight[layer_no].reshape(heads * local_dim, width),
            preferred_element_type=jnp.float32,
        ).reshape(seqs, new_tok, width)
        share_out = lax.psum_scatter(partial_out, "tp", scatter_dimension=2, tiled=True)
        own_cols = lax.dynamic_slice_in_dim(stream, col_start, share_cols, 2)
        stream_share = (own_cols.astype(jnp.float32) + share_out).astype(jnp.bfloat16)
        if layer_no + 1 < layers:
            stream = lax.all_gather(stream_share, "tp", axis=2, tiled=True)
    result = stream_share
    return (result, jnp.stack(new_states))


F32 = jnp.float32
BF16 = jnp.bfloat16


def nt_dot(a, b, precision=None):
    return lax.dot_general(
        a, b, (((1,), (1,)), ((), ())), preferred_element_type=F32, precision=precision
    )


def log2(value):
    return int(value).bit_length() - 1


def rotary_tables(heads, new_tok, head_dim):
    half = head_dim // 2
    freqs = np.power(
        np.float32(ROTARY_BASE), -np.arange(half, dtype=np.float32) * np.float32(2.0 / head_dim)
    ).astype(np.float32)
    tok = np.arange(8) % new_tok
    places = (PAST + tok).astype(np.float32)
    angles = (places[:, None] * freqs[None, :]).astype(np.float32).astype(np.float64)
    gamma = 1.0 - np.power(2.0, -5.0 - np.arange(heads))
    grow = np.power(gamma[:, None], tok[None, :] + 1.0)[:, :, None]
    shrink = head_dim ** (-0.5) / grow
    cosine, sine = np.cos(angles)[None], np.sin(angles)[None]
    block = np.broadcast_to(np.power(gamma, new_tok)[:, None, None], (heads, 8, half))
    return np.stack(
        [cosine * grow, sine * grow, cosine * shrink, sine * shrink, block]
    ).astype(np.float32)


def kernel(
    n, head_dim,
    x_hbm, st_hbm, ng_ref, qw_hbm, kw_hbm, vw_hbm, gw_hbm, gg_ref, ow_hbm, tab_ref,
    y_ref, stv,
    xs, nv, wqk, wvg, wo, qkg, kh, vts, sb, pbs, pbr, yss, ysr, rss, rsr, mkc, mks, fold,
    lsem, ag_s, ag_r, st_s, st_r, pb_s, pb_r, ys_s, ys_r, rs_s, rs_r,
):
    layers, seqs, heads, e_dim, _ = st_hbm.shape
    rows, width = x_hbm.shape
    tok = rows // seqs
    share = width // n
    cols = qw_hbm.shape[2]
    he = heads * e_dim
    half = head_dim // 2
    nc = n // 2
    me = lax.axis_index("tp")
    core = lax.rem(me, 2)
    chip = lax.div(me, 2)
    partner = chip * 2 + 1 - core

    nz = nc // 2
    yy = lax.rem(chip, 2)
    zz = lax.div(chip, 2)

    def at_z(o, y, c):
        return (lax.rem(zz + o + nz, nz) * 2 + y) * 2 + c

    facing = at_z(0, 1 - yy, core)

    def remote(src, dst, ssem, rsem, device):
        return pltpu.make_async_remote_copy(
            src_ref=src, dst_ref=dst, send_sem=ssem, recv_sem=rsem,
            device_id={"tp": device}, device_id_type=pl.DeviceIdType.MESH,
        )

    loads = {}
    count = 0

    def load(name, src, dst):
        nonlocal count
        loads[name] = pltpu.make_async_copy(src, dst, lsem.at[count])
        loads[name].start()
        count += 1

    for j in range(n):
        load(("x", j), x_hbm.at[:, pl.ds(j * share, share)], xs.at[0, j])
    for l in range(layers):
        load(("q", l), qw_hbm.at[l], wqk.at[l, :, pl.ds(0, cols)])
        load(("k", l), kw_hbm.at[l], wqk.at[l, :, pl.ds(cols, cols)])
        load(("v", l), vw_hbm.at[l], wvg.at[l, pl.ds(0, he)])
        load(("g", l), gw_hbm.at[l], wvg.at[l, pl.ds(he, he)])
        load(("s", l), st_hbm.at[l], stv.at[l])
        load(("o", l), ow_hbm.at[l], wo.at[l])

    barrier = pltpu.get_barrier_semaphore()
    for o in range(1, n):
        pl.semaphore_signal(
            barrier, inc=1, device_id={"tp": lax.rem(me + o, n)},
            device_id_type=pl.DeviceIdType.MESH,
        )

    be = seqs * e_dim

    def iota(shape, dim, shift=0):
        return jnp.right_shift(lax.broadcasted_iota(jnp.int32, shape, dim), shift)

    te, tt = log2(e_dim), log2(tok)
    mkc[...] = (iota((rows, be), 0, tt) == iota((rows, be), 1, te)).astype(F32).astype(BF16)
    mks[...] = (iota((be, rows), 0, te) == iota((be, rows), 1, tt)).astype(F32).astype(BF16)
    low = e_dim - 1
    fold[...] = (
        jnp.bitwise_and(iota((be, he), 0), low) == jnp.bitwise_and(iota((be, he), 1), low)
    ).astype(F32).astype(BF16)
    causal = (
        (iota((rows, rows), 0, tt) == iota((rows, rows), 1, tt))
        & (iota((rows, rows), 0) >= iota((rows, rows), 1))
    ).astype(F32)
    heads_of = (iota((heads, he), 0) == iota((heads, he), 1, te)).astype(F32)
    place = (
        iota((e_dim, he), 0) == jnp.bitwise_and(iota((e_dim, he), 1), low)
    ).astype(F32)
    highest = lax.Precision.HIGHEST

    def gather_start(buf, p):
        own = buf.at[me]
        sent = [remote(own, own, ag_s.at[p, nz], ag_r.at[p, nz], facing)]
        for o in range(1, nz):
            sent.append(remote(own, own, ag_s.at[p, o], ag_r.at[p, o], at_z(o, yy, core)))
        sent.append(remote(own, own, ag_s.at[p, nc], ag_r.at[p, nc], partner))
        for copy in sent:
            copy.start()
        return sent

    def gather_finish(buf, p, sent):
        def arrive(slot, k):
            remote(slot, slot, ag_s.at[p, k], ag_r.at[p, k], partner).wait_recv()

        def forward(slot, k, device):
            copy = remote(slot, slot, ag_s.at[p, k], ag_r.at[p, k], device)
            copy.start()
            sent.append(copy)

        for o in range(nz):
            if o:
                slot = buf.at[at_z(-o, yy, core)]
                arrive(slot, o)
                forward(slot, nz + o, facing)
                forward(slot, nc + o, partner)
        for o in range(nz):
            slot = buf.at[at_z(-o, 1 - yy, core)]
            arrive(slot, nz + o)
            forward(slot, nc + nz + o, partner)
        for o in range(nz):
            arrive(buf.at[at_z(-o, yy, 1 - core)], nc + o)
            arrive(buf.at[at_z(-o, 1 - yy, 1 - core)], nc + nz + o)

    def spread(table):
        return jnp.broadcast_to(table[None], (rows // 8, 8, half)).reshape(rows, half)

    started = []
    for l in range(layers):
        if l == 0:
            for j in range(n):
                loads[("x", j)].wait()

        def square(j, acc):
            block = xs[l, j].astype(F32)
            return acc + block * block

        total = lax.fori_loop(0, n, square, jnp.zeros((rows, share), F32))
        scale = lax.rsqrt(jnp.sum(total, axis=1, keepdims=True) / width + EPS_RMS)

        def normalise(j, carry):
            at = pl.ds(pl.multiple_of(j * share, share), share)
            gain = ng_ref[l : l + 1, at].astype(F32)
            nv[:, at] = (xs[l, j].astype(F32) * scale * gain).astype(BF16)
            return carry

        lax.fori_loop(0, n, normalise, 0)
        loads[("q", l)].wait()
        loads[("k", l)].wait()
        qkg[l, me] = jnp.dot(nv[...], wqk[l], preferred_element_type=F32).astype(BF16)
        if l == 0:
            pl.semaphore_wait(barrier, n - 1)
        sent = gather_start(qkg.at[l], 2 * l)
        loads[("v", l)].wait()
        loads[("g", l)].wait()
        vg = nt_dot(nv[...], wvg[l])
        values = vg[:, :he].astype(BF16)
        gates = vg[:, he:].astype(BF16).astype(F32)
        vts[...] = jnp.transpose(values.astype(F32)).astype(BF16)
        loads[("s", l)].wait()
        gather_finish(qkg.at[l], 2 * l, sent)
        started += sent

        def mix(h, acc):
            qk_a = qkg[l, 2 * h].astype(F32)
            qk_b = qkg[l, 2 * h + 1].astype(F32)
            qa, ka = qk_a[:, :half], qk_a[:, half:]
            qb, kb = qk_b[:, :half], qk_b[:, half:]
            cq, sq = spread(tab_ref[0, h]), spread(tab_ref[1, h])
            ck, sk = spread(tab_ref[2, h]), spread(tab_ref[3, h])
            rq = jnp.concatenate([qa * cq - qb * sq, qb * cq + qa * sq], axis=1).astype(BF16)
            rk = jnp.concatenate([ka * ck - kb * sk, kb * ck + ka * sk], axis=1).astype(BF16)
            kh[h] = rk
            state = stv[l, :, h].reshape(be, head_dim).astype(BF16)
            scores = (nt_dot(rq, rk) * causal).astype(BF16)
            carried = nt_dot(rq, state).astype(BF16) * mkc[...]
            part = jnp.dot(scores, values, preferred_element_type=F32)
            part = part + jnp.dot(carried, fold[...], preferred_element_type=F32)
            own = (iota((1, he), 1, te) == h).astype(F32)
            return acc + part * own

        mixed = lax.fori_loop(0, heads, mix, jnp.zeros((rows, he), F32))
        sums = nt_dot(heads_of, mixed, highest)
        squares = nt_dot(heads_of, mixed * mixed, highest)
        sb[l, me] = jnp.concatenate([sums, squares], axis=0)
        sent = []
        for o in range(1, n):
            sent.append(
                remote(sb.at[l, me], sb.at[l, me], st_s.at[l, o], st_r.at[l, o], lax.rem(me + o, n))
            )
        for copy in sent:
            copy.start()
        started += sent

        def update(h, carry):
            at = pl.ds(pl.multiple_of(h * e_dim, e_dim), e_dim)
            tall = jnp.broadcast_to(vts[at, :][None], (seqs, e_dim, rows)).reshape(be, rows)
            fresh = jnp.dot(tall * mks[...], kh[h], preferred_element_type=F32)
            row = tab_ref[4, h][0:1, :]
            fade = jnp.concatenate([row, row], axis=1)
            state = stv[l, :, h].reshape(be, head_dim)
            stv[l, :, h] = ((state + fresh) * fade).reshape(seqs, e_dim, head_dim)
            return carry

        lax.fori_loop(0, heads, update, 0)

        for o in range(1, n):
            slot = sb.at[l, lax.rem(me - o + n, n)]
            remote(slot, slot, st_s.at[l, o], st_r.at[l, o], partner).wait_recv()
        stats = jnp.sum(sb[l], axis=0)
        mean = stats[:heads] / head_dim
        var = stats[heads:] / head_dim - mean * mean
        rstd = lax.rsqrt(var + EPS_GROUP)

        def expand(small):
            return lax.dot_general(
                small, heads_of, (((0,), (0,)), ((), ())),
                preferred_element_type=F32, precision=highest,
            )

        gain = jnp.dot(gg_ref[l].astype(F32), place, preferred_element_type=F32, precision=highest)
        gain = jnp.sum(gain * heads_of, axis=0, keepdims=True)
        normal = (mixed - expand(mean)) * expand(rstd) * gain
        gated = (gates / (1.0 + jnp.exp(-gates)) * normal).astype(BF16)

        loads[("o", l)].wait()

        def chunk(j):
            at = pl.ds(pl.multiple_of(j * share, share), share)
            return jnp.dot(gated, wo[l, :, at], preferred_element_type=F32)

        order = list(range(1, nz)) + [0]
        for side in (1, 0):
            for o in order:
                k = side * nz + o
                y = 1 - yy if side else yy
                pbs[l, k] = chunk(at_z(o, y, 1 - core)).astype(BF16)
                copy = remote(pbs.at[l, k], pbr.at[l, k], pb_s.at[l, k], pb_r.at[l, k], partner)
                copy.start()
                started.append(copy)

        def paired(o, side):
            k = side * nz + o
            own = chunk(at_z(o, 1 - yy if side else yy, core))
            remote(pbs.at[l, k], pbr.at[l, k], pb_s.at[l, k], pb_r.at[l, k], partner).wait_recv()
            return own + pbr[l, k].astype(F32)

        for o in order:
            yss[l, o] = paired(o, 1).astype(BF16)
            copy = remote(yss.at[l, o], ysr.at[l, o], ys_s.at[l, o], ys_r.at[l, o], facing)
            copy.start()
            started.append(copy)
        acc = None
        for o in order:
            own = paired(o, 0)
            remote(yss.at[l, o], ysr.at[l, o], ys_s.at[l, o], ys_r.at[l, o], facing).wait_recv()
            own = own + ysr[l, o].astype(F32)
            if o:
                rss[l, o] = own.astype(BF16)
                copy = remote(
                    rss.at[l, o], rsr.at[l, o], rs_s.at[l, o], rs_r.at[l, o], at_z(o, yy, core)
                )
                copy.start()
                started.append(copy)
            else:
                acc = own
        for o in range(1, nz):
            remote(rss.at[l, o], rsr.at[l, o], rs_s.at[l, o], rs_r.at[l, o], facing).wait_recv()
            acc = acc + rsr[l, o].astype(F32)
        fresh_x = (xs[l, me].astype(F32) + acc).astype(BF16)
        if l + 1 < layers:
            xs[l + 1, me] = fresh_x
            sent = gather_start(xs.at[l + 1], 2 * l + 1)
            gather_finish(xs.at[l + 1], 2 * l + 1, sent)
            started += sent
        else:
            y_ref[...] = fresh_x
    for copy in started:
        copy.wait_send()


def store_kernel(y_ref, state_ref, y_out, state_out, sem):
    copies = [
        pltpu.make_async_copy(state_ref.at[l], state_out.at[l], sem.at[l])
        for l in range(state_ref.shape[0])
    ]
    for copy in copies:
        copy.start()
    y_out[...] = y_ref[...]
    for copy in copies:
        copy.wait()


def local(
    stream_in, state_in, norm_gain, query_weight, key_weight,
    value_weight, gate_weight, group_gain, output_weight,
):
    n = lax.axis_size("tp")
    seqs, tok, width = stream_in.shape
    layers, _, heads, e_dim, head_dim = state_in.shape
    cols = query_weight.shape[2]
    rows = seqs * tok
    he = heads * e_dim
    share = width // n
    fits = (
        cols == 128 and head_dim == 256 and he == 128 and heads == 8 and e_dim == 16
        and share % 128 == 0 and n % 4 == 0 and rows == 128 and 8 % tok == 0
    )
    if not fits:
        return plain_local(
            stream_in, state_in, norm_gain, query_weight, key_weight,
            value_weight, gate_weight, group_gain, output_weight,
        )
    nc = n // 2
    be = seqs * e_dim
    hbm = pl.BlockSpec(memory_space=pl.ANY)
    vmem = pl.BlockSpec(memory_space=pltpu.VMEM)
    dma = pltpu.SemaphoreType.DMA
    tables = jnp.asarray(rotary_tables(heads, tok, head_dim))
    flat = lambda w: jnp.transpose(w, (0, 2, 3, 1)).reshape(layers, he, width)
    y, new_state = pl.pallas_call(
        functools.partial(kernel, n, head_dim),
        name="retention",
        out_shape=(
            jax.ShapeDtypeStruct((rows, share), BF16),
            pltpu.VMEM(state_in.shape, F32),
        ),
        in_specs=[hbm, hbm, vmem, hbm, hbm, hbm, hbm, vmem, hbm, vmem],
        out_specs=(vmem, vmem),
        scratch_shapes=[
            pltpu.VMEM((layers, n, rows, share), BF16),
            pltpu.VMEM((rows, width), BF16),
            pltpu.VMEM((layers, width, 2 * cols), BF16),
            pltpu.VMEM((layers, 2 * he, width), BF16),
            pltpu.VMEM((layers, he, width), BF16),
            pltpu.VMEM((layers, n, rows, 2 * cols), BF16),
            pltpu.VMEM((heads, rows, head_dim), BF16),
            pltpu.VMEM((he, rows), BF16),
            pltpu.VMEM((layers, n, 2 * heads, rows), F32),
            pltpu.VMEM((layers, nc, rows, share), BF16),
            pltpu.VMEM((layers, nc, rows, share), BF16),
            pltpu.VMEM((layers, nc // 2, rows, share), BF16),
            pltpu.VMEM((layers, nc // 2, rows, share), BF16),
            pltpu.VMEM((layers, nc // 2, rows, share), BF16),
            pltpu.VMEM((layers, nc // 2, rows, share), BF16),
            pltpu.VMEM((rows, be), BF16),
            pltpu.VMEM((be, rows), BF16),
            pltpu.VMEM((be, he), BF16),
            dma((n + 6 * layers,)),
            dma((2 * layers, n)),
            dma((2 * layers, n)),
            dma((layers, n)),
            dma((layers, n)),
            dma((layers, nc)),
            dma((layers, nc)),
            dma((layers, nc // 2)),
            dma((layers, nc // 2)),
            dma((layers, nc // 2)),
            dma((layers, nc // 2)),
        ],
        compiler_params=pltpu.CompilerParams(
            collective_id=0, has_side_effects=True, vmem_limit_bytes=44 * 2**20
        ),
    )(
        stream_in.reshape(rows, width), state_in, norm_gain, query_weight, key_weight,
        flat(value_weight), flat(gate_weight), group_gain,
        output_weight.reshape(layers, he, width), tables,
    )
    y, new_state = pl.pallas_call(
        store_kernel,
        name="store",
        out_shape=(
            jax.ShapeDtypeStruct((rows, share), BF16),
            jax.ShapeDtypeStruct(state_in.shape, F32),
        ),
        in_specs=[vmem, hbm],
        out_specs=(vmem, hbm),
        scratch_shapes=[dma((layers,))],
        compiler_params=pltpu.CompilerParams(vmem_limit_bytes=2 * 2**20),
    )(y, new_state)
    return y.reshape(seqs, tok, share), new_state


def solution(mesh):
    in_specs = (
        P("grp", None, None),
        P(None, "grp", None, "tp", None),
        P(),
        P(None, None, "tp"),
        P(None, None, "tp"),
        P(None, None, None, "tp"),
        P(None, None, None, "tp"),
        P(None, None, "tp"),
        P(None, None, "tp", None),
    )
    out_specs = (P("grp", None, "tp"), P(None, "grp", None, "tp", None))
    return jax.shard_map(local, mesh=mesh, in_specs=in_specs, out_specs=out_specs, check_vma=False)
```

```python
import functools

import jax
import jax.numpy as jnp
import numpy as np
from jax import lax
from jax.experimental import pallas as pl
from jax.experimental.pallas import tpu as pltpu
from jax.sharding import PartitionSpec as P

HEAD_DIM = 256
PAST = 1024


EPS_RMS = 1e-06
EPS_GROUP = 1e-05
ROTARY_BASE = 10000.0


def log_decays(count):
    return jnp.log(1.0 - jnp.power(2.0, -5.0 - jnp.arange(count, dtype=jnp.float32)))


def decay_tables(log_gamma, count):
    steps = jnp.arange(count, dtype=jnp.float32)
    gap = steps[:, None] - steps[None, :]
    intra = jnp.where(
        gap[None] >= 0, jnp.exp(log_gamma[:, None, None] * jnp.maximum(gap, 0.0)[None]), 0.0
    )
    q_decay = jnp.exp(log_gamma[None, :] * (steps[:, None] + 1.0))
    k_decay = jnp.exp(log_gamma[None, :] * (count - 1.0 - steps[:, None]))
    block_decay = jnp.exp(log_gamma * count)
    return (intra, q_decay, k_decay, block_decay)


def rotate(values, offset):
    half_dim = values.shape[-1] // 2
    freqs = jnp.power(
        ROTARY_BASE, -jnp.arange(half_dim, dtype=jnp.float32) * (2.0 / values.shape[-1])
    )
    places = (offset + jnp.arange(values.shape[1])).astype(jnp.float32)
    angles = places[:, None] * freqs[None, :]
    cosine = jnp.cos(angles)[None, :, None, :]
    sine = jnp.sin(angles)[None, :, None, :]
    first = values[..., :half_dim]
    second = values[..., half_dim:]
    return jnp.concatenate(
        [first * cosine - second * sine, second * cosine + first * sine], axis=-1
    )


def plain_local(
    stream_in,
    state_in,
    norm_gain,
    query_weight,
    key_weight,
    value_weight,
    gate_weight,
    group_gain,
    output_weight,
):
    seqs, new_tok, width = stream_in.shape
    heads, local_dim = (value_weight.shape[2], value_weight.shape[3])
    head_dim = HEAD_DIM
    log_gamma = log_decays(heads)
    intra, q_decay, k_decay, block_decay = decay_tables(log_gamma, new_tok)
    highest = lax.Precision.HIGHEST
    share_cols = width // lax.axis_size("tp")
    col_start = lax.axis_index("tp") * share_cols
    layers = state_in.shape[0]
    stream = stream_in
    stream_share = stream_in
    new_states = []
    for layer_no in range(layers):
        stream_f = stream.astype(jnp.float32)
        normed = stream_f * lax.rsqrt(
            jnp.mean(stream_f * stream_f, axis=-1, keepdims=True) + EPS_RMS
        )
        normed = (normed * norm_gain[layer_no].astype(jnp.float32)).astype(jnp.bfloat16)
        flat = normed.reshape(seqs * new_tok, width)
        query_part = jnp.dot(flat, query_weight[layer_no], preferred_element_type=jnp.float32)
        query_part = query_part.astype(jnp.bfloat16).reshape(seqs, new_tok, -1)
        key_part = jnp.dot(flat, key_weight[layer_no], preferred_element_type=jnp.float32)
        key_part = key_part.astype(jnp.bfloat16).reshape(seqs, new_tok, -1)

        def project_local(weight):
            result = jnp.dot(
                flat, weight.reshape(width, heads * local_dim), preferred_element_type=jnp.float32
            )
            result = lax.optimization_barrier(result.astype(jnp.bfloat16))
            return result.astype(jnp.float32).reshape(seqs, new_tok, heads, local_dim)

        values_f = project_local(value_weight[layer_no])
        gates_f = project_local(gate_weight[layer_no])
        queries, key_rows = (
            lax.all_gather(query_part, "tp", axis=2, tiled=True),
            lax.all_gather(key_part, "tp", axis=2, tiled=True),
        )
        queries = queries.astype(jnp.float32).reshape(seqs, new_tok, heads, head_dim)
        key_rows = key_rows.astype(jnp.float32).reshape(seqs, new_tok, heads, head_dim)
        rot_q = rotate(queries, PAST)
        rot_k = rotate(key_rows, PAST) * head_dim ** (-0.5)
        scores = jnp.einsum("bthd,bshd->bhts", rot_q, rot_k, precision=highest) * intra[None]
        inner = jnp.einsum("bhts,bshe->bthe", scores, values_f, precision=highest)
        state = state_in[layer_no]
        carried = (
            jnp.einsum("bthd,bhed->bthe", rot_q, state, precision=highest)
            * q_decay[None, :, :, None]
        )
        mixed = inner + carried
        new_state = state * block_decay[None, :, None, None] + jnp.einsum(
            "bthe,bthd->bhed", values_f, rot_k * k_decay[None, :, :, None], precision=highest
        )
        new_states.append(new_state)
        totals, squares = lax.psum((jnp.sum(mixed, axis=-1), jnp.sum(mixed * mixed, axis=-1)), "tp")
        mean_o = (totals / head_dim)[..., None]
        var_o = (squares / head_dim)[..., None] - mean_o * mean_o
        normal = (
            (mixed - mean_o)
            * lax.rsqrt(var_o + EPS_GROUP)
            * group_gain[layer_no].astype(jnp.float32)[None, None]
        )
        gated = (jax.nn.silu(gates_f) * normal).astype(jnp.bfloat16)
        partial_out = jnp.dot(
            gated.reshape(seqs * new_tok, heads * local_dim),
            output_weight[layer_no].reshape(heads * local_dim, width),
            preferred_element_type=jnp.float32,
        ).reshape(seqs, new_tok, width)
        share_out = lax.psum_scatter(partial_out, "tp", scatter_dimension=2, tiled=True)
        own_cols = lax.dynamic_slice_in_dim(stream, col_start, share_cols, 2)
        stream_share = (own_cols.astype(jnp.float32) + share_out).astype(jnp.bfloat16)
        if layer_no + 1 < layers:
            stream = lax.all_gather(stream_share, "tp", axis=2, tiled=True)
    result = stream_share
    return (result, jnp.stack(new_states))


LAG = 0
F32 = jnp.float32
BF16 = jnp.bfloat16


def nt_dot(a, b, precision=None):
    return lax.dot_general(
        a, b, (((1,), (1,)), ((), ())), preferred_element_type=F32, precision=precision
    )


def log2(value):
    return int(value).bit_length() - 1


def rotary_tables(heads, new_tok, head_dim):
    half = head_dim // 2
    freqs = np.power(
        np.float32(ROTARY_BASE), -np.arange(half, dtype=np.float32) * np.float32(2.0 / head_dim)
    ).astype(np.float32)
    tok = np.arange(8) % new_tok
    places = (PAST + tok).astype(np.float32)
    angles = (places[:, None] * freqs[None, :]).astype(np.float32).astype(np.float64)
    gamma = 1.0 - np.power(2.0, -5.0 - np.arange(heads))
    grow = np.power(gamma[:, None], tok[None, :] + 1.0)[:, :, None]
    shrink = head_dim ** (-0.5) / grow
    cosine, sine = np.cos(angles)[None], np.sin(angles)[None]
    block = np.broadcast_to(np.power(gamma, new_tok)[:, None, None], (heads, 8, half))
    return np.stack(
        [cosine * grow, sine * grow, cosine * shrink, sine * shrink, block]
    ).astype(np.float32)


def kernel(
    n, head_dim, groups, lag,
    x_hbm, st_hbm, ng_ref, qw_hbm, kw_hbm, vw_hbm, gw_hbm, gg_ref, ow_hbm, tab_ref,
    y_ref, stv,
    xs, nv, wqk, wvg, wo, qkg, kh, vts, sb, pbs, pbr, yss, ysr, rss, rsr, mkc, mks, fold,
    lsem, ag_s, ag_r, st_s, st_r, pb_s, pb_r, ys_s, ys_r, rs_s, rs_r,
):
    layers, seqs, heads, e_dim, _ = st_hbm.shape
    tok = x_hbm.shape[0] // seqs
    width = x_hbm.shape[1]
    seqs = seqs // groups
    rows = seqs * tok
    share = width // n
    cols = qw_hbm.shape[2]
    he = heads * e_dim
    half = head_dim // 2
    nc = n // 2
    me = lax.axis_index("tp")
    core = lax.rem(me, 2)
    chip = lax.div(me, 2)
    partner = chip * 2 + 1 - core

    nz = nc // 2
    yy = lax.rem(chip, 2)
    zz = lax.div(chip, 2)

    def at_z(o, y, c):
        z, bit = zz, 1
        while bit < nz:
            if o & bit:
                z = z + bit - 2 * bit * lax.rem(lax.div(z, bit), 2)
            bit = 2 * bit
        return (z * 2 + y) * 2 + c

    facing = at_z(0, 1 - yy, core)
    far = list(range(2, nz)) + [1]

    def remote(src, dst, ssem, rsem, device):
        return pltpu.make_async_remote_copy(
            src_ref=src, dst_ref=dst, send_sem=ssem, recv_sem=rsem,
            device_id={"tp": device}, device_id_type=pl.DeviceIdType.MESH,
        )

    loads = {}
    count = 0

    def load(name, src, dst):
        nonlocal count
        loads[name] = pltpu.make_async_copy(src, dst, lsem.at[count])
        loads[name].start()
        count += 1

    for g in range(groups):
        for j in range(n):
            source = x_hbm.at[pl.ds(g * rows, rows), pl.ds(j * share, share)]
            load(("x", g, j), source, xs.at[g, j])
    for l in range(layers):
        load(("q", l), qw_hbm.at[l], wqk.at[l, :, pl.ds(0, cols)])
        load(("k", l), kw_hbm.at[l], wqk.at[l, :, pl.ds(cols, cols)])
        load(("v", l), vw_hbm.at[l], wvg.at[l, pl.ds(0, he)])
        load(("g", l), gw_hbm.at[l], wvg.at[l, pl.ds(he, he)])
        load(("s", l), st_hbm.at[l], stv.at[l])
        load(("o", l), ow_hbm.at[l], wo.at[l])

    barrier = pltpu.get_barrier_semaphore()
    for o in range(1, n):
        pl.semaphore_signal(
            barrier, inc=1, device_id={"tp": lax.rem(me + o, n)},
            device_id_type=pl.DeviceIdType.MESH,
        )

    be = seqs * e_dim

    def iota(shape, dim, shift=0):
        return jnp.right_shift(lax.broadcasted_iota(jnp.int32, shape, dim), shift)

    te, tt = log2(e_dim), log2(tok)
    mkc[...] = (iota((rows, be), 0, tt) == iota((rows, be), 1, te)).astype(F32).astype(BF16)
    mks[...] = (iota((be, rows), 0, te) == iota((be, rows), 1, tt)).astype(F32).astype(BF16)
    low = e_dim - 1
    fold[...] = (
        jnp.bitwise_and(iota((be, he), 0), low) == jnp.bitwise_and(iota((be, he), 1), low)
    ).astype(F32).astype(BF16)
    causal = (
        (iota((rows, rows), 0, tt) == iota((rows, rows), 1, tt))
        & (iota((rows, rows), 0) >= iota((rows, rows), 1))
    ).astype(F32)
    heads_of = (iota((heads, he), 0) == iota((heads, he), 1, te)).astype(F32)
    place = (
        iota((e_dim, he), 0) == jnp.bitwise_and(iota((e_dim, he), 1), low)
    ).astype(F32)
    highest = lax.Precision.HIGHEST

    def gather_start(buf, p):
        own = buf.at[me]
        sent = [remote(own, own, ag_s.at[p, nz], ag_r.at[p, nz], facing)]
        for o in far:
            sent.append(remote(own, own, ag_s.at[p, o], ag_r.at[p, o], at_z(o, yy, core)))
        sent.append(remote(own, own, ag_s.at[p, nc], ag_r.at[p, nc], partner))
        for copy in sent:
            copy.start()
        return sent

    def gather_finish(buf, p, sent):
        def arrive(slot, k):
            remote(slot, slot, ag_s.at[p, k], ag_r.at[p, k], partner).wait_recv()

        def forward(slot, k, device):
            copy = remote(slot, slot, ag_s.at[p, k], ag_r.at[p, k], device)
            copy.start()
            sent.append(copy)

        for o in range(1, nz):
            slot = buf.at[at_z(o, yy, core)]
            arrive(slot, o)
            forward(slot, nz + o, facing)
            forward(slot, nc + o, partner)
        yield
        for o in range(nz):
            slot = buf.at[at_z(o, 1 - yy, core)]
            arrive(slot, nz + o)
            forward(slot, nc + nz + o, partner)
        yield
        for o in range(nz):
            arrive(buf.at[at_z(o, yy, 1 - core)], nc + o)
            arrive(buf.at[at_z(o, 1 - yy, 1 - core)], nc + nz + o)

    def spread(table):
        return jnp.broadcast_to(table[None], (rows // 8, 8, half)).reshape(rows, half)

    started = []
    waited = set()

    def once(key):
        if key not in waited:
            waited.add(key)
            loads[key].wait()

    def chain(g):
        mine = pl.ds(g * seqs, seqs)
        for l in range(layers):
            lg = l * groups + g
            if l == 0:
                for j in range(n):
                    loads[("x", g, j)].wait()

            def square(j, acc):
                block = xs[lg, j].astype(F32)
                return acc + block * block

            total = lax.fori_loop(0, n, square, jnp.zeros((rows, share), F32))
            scale = lax.rsqrt(jnp.sum(total, axis=1, keepdims=True) / width + EPS_RMS)

            def normalise(j, carry):
                at = pl.ds(pl.multiple_of(j * share, share), share)
                gain = ng_ref[l : l + 1, at].astype(F32)
                nv[g, :, at] = (xs[lg, j].astype(F32) * scale * gain).astype(BF16)
                return carry

            lax.fori_loop(0, n, normalise, 0)
            once(("q", l))
            once(("k", l))
            qkg[lg, me] = jnp.dot(nv[g], wqk[l], preferred_element_type=F32).astype(BF16)
            if l == 0 and g == 0:
                pl.semaphore_wait(barrier, n - 1)
            sent = gather_start(qkg.at[lg], lg)
            once(("v", l))
            once(("g", l))
            vg = nt_dot(nv[g], wvg[l])
            values = vg[:, :he].astype(BF16)
            gates = vg[:, he:].astype(BF16).astype(F32)
            vts[g] = jnp.transpose(values.astype(F32)).astype(BF16)
            once(("s", l))
            yield
            yield from gather_finish(qkg.at[lg], lg, sent)
            started.extend(sent)

            def mix(h, acc):
                qk_a = qkg[lg, 2 * h].astype(F32)
                qk_b = qkg[lg, 2 * h + 1].astype(F32)
                qa, ka = qk_a[:, :half], qk_a[:, half:]
                qb, kb = qk_b[:, :half], qk_b[:, half:]
                cq, sq = spread(tab_ref[0, h]), spread(tab_ref[1, h])
                ck, sk = spread(tab_ref[2, h]), spread(tab_ref[3, h])
                rq = jnp.concatenate([qa * cq - qb * sq, qb * cq + qa * sq], axis=1).astype(BF16)
                rk = jnp.concatenate([ka * ck - kb * sk, kb * ck + ka * sk], axis=1).astype(BF16)
                kh[g * heads + h] = rk
                state = stv[l, mine, h].reshape(be, head_dim).astype(BF16)
                scores = (nt_dot(rq, rk) * causal).astype(BF16)
                carried = nt_dot(rq, state).astype(BF16) * mkc[...]
                part = jnp.dot(scores, values, preferred_element_type=F32)
                part = part + jnp.dot(carried, fold[...], preferred_element_type=F32)
                own = (iota((1, he), 1, te) == h).astype(F32)
                return acc + part * own

            mixed = lax.fori_loop(0, heads, mix, jnp.zeros((rows, he), F32), unroll=True)
            sums = nt_dot(heads_of, mixed, highest)
            squares = nt_dot(heads_of, mixed * mixed, highest)
            sb[lg, me] = jnp.concatenate([sums, squares], axis=1)
            sent = []
            for o in range(1, n):
                sent.append(
                    remote(sb.at[lg, me], sb.at[lg, me], st_s.at[lg, o], st_r.at[lg, o], lax.rem(me + o, n))
                )
            for copy in sent:
                copy.start()
            started.extend(sent)

            def update(h, carry):
                at = pl.ds(pl.multiple_of(h * e_dim, e_dim), e_dim)
                tall = jnp.broadcast_to(vts[g, at, :][None], (seqs, e_dim, rows)).reshape(be, rows)
                fresh = jnp.dot(tall * mks[...], kh[g * heads + h], preferred_element_type=F32)
                row = tab_ref[4, h][0:1, :]
                fade = jnp.concatenate([row, row], axis=1)
                state = stv[l, mine, h].reshape(be, head_dim)
                stv[l, mine, h] = ((state + fresh) * fade).reshape(seqs, e_dim, head_dim)
                return carry

            lax.fori_loop(0, heads, update, 0, unroll=True)
            yield

            for o in range(1, n):
                slot = sb.at[lg, lax.rem(me - o + n, n)]
                remote(slot, slot, st_s.at[lg, o], st_r.at[lg, o], partner).wait_recv()
            stats = jnp.sum(sb[lg], axis=0)
            mean = stats[:, :rows] / head_dim
            var = stats[:, rows:] / head_dim - mean * mean
            rstd = lax.rsqrt(var + EPS_GROUP)

            def expand(small):
                return lax.dot_general(
                    small, heads_of, (((0,), (0,)), ((), ())),
                    preferred_element_type=F32, precision=highest,
                )

            gain = jnp.dot(gg_ref[l].astype(F32), place, preferred_element_type=F32, precision=highest)
            gain = jnp.sum(gain * heads_of, axis=0, keepdims=True)
            normal = (mixed - expand(mean)) * expand(rstd) * gain
            gated = (gates / (1.0 + jnp.exp(-gates)) * normal).astype(BF16)

            once(("o", l))

            def chunk(j):
                at = pl.ds(pl.multiple_of(j * share, share), share)
                return jnp.dot(gated, wo[l, :, at], preferred_element_type=F32)

            order = far + [0]
            for side in (1, 0):
                for o in order:
                    k = side * nz + o
                    y = 1 - yy if side else yy
                    pbs[lg, k] = chunk(at_z(o, y, 1 - core)).astype(BF16)
                    copy = remote(pbs.at[lg, k], pbr.at[lg, k], pb_s.at[lg, k], pb_r.at[lg, k], partner)
                    copy.start()
                    started.append(copy)

            yield

            def paired(o, side):
                k = side * nz + o
                own = chunk(at_z(o, 1 - yy if side else yy, core))
                remote(pbs.at[lg, k], pbr.at[lg, k], pb_s.at[lg, k], pb_r.at[lg, k], partner).wait_recv()
                return own + pbr[lg, k].astype(F32)

            for o in order:
                yss[lg, o] = paired(o, 1).astype(BF16)
                copy = remote(yss.at[lg, o], ysr.at[lg, o], ys_s.at[lg, o], ys_r.at[lg, o], facing)
                copy.start()
                started.append(copy)
            yield
            acc = None
            for o in order:
                own = paired(o, 0)
                remote(yss.at[lg, o], ysr.at[lg, o], ys_s.at[lg, o], ys_r.at[lg, o], facing).wait_recv()
                own = own + ysr[lg, o].astype(F32)
                if o:
                    rss[lg, o] = own.astype(BF16)
                    copy = remote(
                        rss.at[lg, o], rsr.at[lg, o], rs_s.at[lg, o], rs_r.at[lg, o], at_z(o, yy, core)
                    )
                    copy.start()
                    started.append(copy)
                else:
                    acc = own
            yield
            for o in range(1, nz):
                remote(rss.at[lg, o], rsr.at[lg, o], rs_s.at[lg, o], rs_r.at[lg, o], facing).wait_recv()
                acc = acc + rsr[lg, o].astype(F32)
            fresh_x = (xs[lg, me].astype(F32) + acc).astype(BF16)
            if l + 1 < layers:
                xs[lg + groups, me] = fresh_x
                sent = gather_start(xs.at[lg + groups], layers * groups + lg)
                yield
                yield from gather_finish(xs.at[lg + groups], layers * groups + lg, sent)
                started.extend(sent)
            else:
                y_ref[pl.ds(g * rows, rows), :] = fresh_x

    chains = [chain(g) for g in range(groups)]
    live = list(range(groups))
    step = 0
    while live:
        for g in list(live):
            if step >= lag * g and next(chains[g], live) is live:
                live.remove(g)
        step += 1
    for copy in started:
        copy.wait_send()


def store_kernel(y_ref, state_ref, y_out, state_out, sem):
    copies = [
        pltpu.make_async_copy(state_ref.at[l], state_out.at[l], sem.at[l])
        for l in range(state_ref.shape[0])
    ]
    for copy in copies:
        copy.start()
    y_out[...] = y_ref[...]
    for copy in copies:
        copy.wait()


def local(
    stream_in, state_in, norm_gain, query_weight, key_weight,
    value_weight, gate_weight, group_gain, output_weight,
):
    n = lax.axis_size("tp")
    seqs, tok, width = stream_in.shape
    layers, _, heads, e_dim, head_dim = state_in.shape
    cols = query_weight.shape[2]
    rows = seqs * tok
    he = heads * e_dim
    share = width // n
    fits = (
        cols == 128 and head_dim == 256 and he == 128 and heads == 8 and e_dim == 16
        and share % 128 == 0 and n % 4 == 0 and n & (n - 1) == 0 and rows == 128 and 8 % tok == 0
    )
    if not fits:
        return plain_local(
            stream_in, state_in, norm_gain, query_weight, key_weight,
            value_weight, gate_weight, group_gain, output_weight,
        )
    groups = 1
    nc = n // 2
    part = rows // groups
    be = seqs * e_dim // groups
    steps = layers * groups
    hbm = pl.BlockSpec(memory_space=pl.ANY)
    vmem = pl.BlockSpec(memory_space=pltpu.VMEM)
    dma = pltpu.SemaphoreType.DMA
    tables = jnp.asarray(rotary_tables(heads, tok, head_dim))
    flat = lambda w: jnp.transpose(w, (0, 2, 3, 1)).reshape(layers, he, width)
    y, new_state = pl.pallas_call(
        functools.partial(kernel, n, head_dim, groups, LAG),
        name="retention",
        out_shape=(
            jax.ShapeDtypeStruct((rows, share), BF16),
            pltpu.VMEM(state_in.shape, F32),
        ),
        in_specs=[hbm, hbm, vmem, hbm, hbm, hbm, hbm, vmem, hbm, vmem],
        out_specs=(vmem, vmem),
        scratch_shapes=[
            pltpu.VMEM((steps, n, part, share), BF16),
            pltpu.VMEM((groups, part, width), BF16),
            pltpu.VMEM((layers, width, 2 * cols), BF16),
            pltpu.VMEM((layers, 2 * he, width), BF16),
            pltpu.VMEM((layers, he, width), BF16),
            pltpu.VMEM((steps, n, part, 2 * cols), BF16),
            pltpu.VMEM((groups * heads, part, head_dim), BF16),
            pltpu.VMEM((groups, he, part), BF16),
            pltpu.VMEM((steps, n, heads, 2 * part), F32),
            pltpu.VMEM((steps, nc, part, share), BF16),
            pltpu.VMEM((steps, nc, part, share), BF16),
            pltpu.VMEM((steps, nc // 2, part, share), BF16),
            pltpu.VMEM((steps, nc // 2, part, share), BF16),
            pltpu.VMEM((steps, nc // 2, part, share), BF16),
            pltpu.VMEM((steps, nc // 2, part, share), BF16),
            pltpu.VMEM((part, be), BF16),
            pltpu.VMEM((be, part), BF16),
            pltpu.VMEM((be, he), BF16),
            dma((groups * n + 6 * layers,)),
            dma((2 * steps, n)),
            dma((2 * steps, n)),
            dma((steps, n)),
            dma((steps, n)),
            dma((steps, nc)),
            dma((steps, nc)),
            dma((steps, nc // 2)),
            dma((steps, nc // 2)),
            dma((steps, nc // 2)),
            dma((steps, nc // 2)),
        ],
        compiler_params=pltpu.CompilerParams(
            collective_id=0, has_side_effects=True, vmem_limit_bytes=44 * 2**20
        ),
    )(
        stream_in.reshape(rows, width), state_in, norm_gain, query_weight, key_weight,
        flat(value_weight), flat(gate_weight), group_gain,
        output_weight.reshape(layers, he, width), tables,
    )
    y, new_state = pl.pallas_call(
        store_kernel,
        name="store",
        out_shape=(
            jax.ShapeDtypeStruct((rows, share), BF16),
            jax.ShapeDtypeStruct(state_in.shape, F32),
        ),
        in_specs=[vmem, hbm],
        out_specs=(vmem, hbm),
        scratch_shapes=[dma((layers,))],
        compiler_params=pltpu.CompilerParams(vmem_limit_bytes=2 * 2**20),
    )(y, new_state)
    return y.reshape(seqs, tok, share), new_state


def solution(mesh):
    in_specs = (
        P("grp", None, None),
        P(None, "grp", None, "tp", None),
        P(),
        P(None, None, "tp"),
        P(None, None, "tp"),
        P(None, None, None, "tp"),
        P(None, None, None, "tp"),
        P(None, None, "tp"),
        P(None, None, "tp", None),
    )
    out_specs = (P("grp", None, "tp"), P(None, "grp", None, "tp", None))
    return jax.shard_map(local, mesh=mesh, in_specs=in_specs, out_specs=out_specs, check_vma=False)
```
